1024 devices in a mesh: kv: 256 (over z, x, core), tp: 4 (over y).
Axes of the slice: x: 4, y: 4, z: 32, core: 2. Of those that a mesh axis runs over, the one named last changes fastest.
Arguments:
- hidden_in: bfloat16 [4, 16384, 2048], P(None, 'kv'), may hold values from -84 to 84
- w_query: bfloat16 [2048, 1024], P(None, 'tp'), may hold values from -0.125 to 0.125
- w_cmp_key: bfloat16 [2048, 256], P(None, 'tp'), may hold values from -0.125 to 0.125
- w_cmp_value: bfloat16 [2048, 256], P(None, 'tp'), may hold values from -0.8838835 to 0.8838835
- w_sel_key: bfloat16 [2048, 256], P(None, 'tp'), may hold values from -0.125 to 0.125
- w_sel_value: bfloat16 [2048, 256], P(None, 'tp'), may hold values from -0.8838835 to 0.8838835
- w_gate: bfloat16 [2048, 2, 16], replicated, may hold values from -0.125 to 0.125
- cmp_key_in: bfloat16 [2048, 128], replicated, may hold values from -0.125 to 0.125
- cmp_key_out: bfloat16 [128, 64], replicated, may hold values from -0.5 to 0.5
- cmp_value_in: bfloat16 [2048, 128], replicated, may hold values from -0.125 to 0.125
- cmp_value_out: bfloat16 [128, 64], replicated, may hold values from -0.5 to 0.5
- out_gain: float32 [1024], replicated, may hold values from 0.1 to 1.9
- w_out: bfloat16 [1024, 2048], replicated, may hold values from -0.1875 to 0.1875
- seq_lengths: int32 [4], replicated, may hold values from 1 to 16384, 26214 in all
- chosen: int32 [4, 256, 4, 16], P(None, 'kv', 'tp'), may hold values from -1 to 255, as said below
Outputs:
- attended: bfloat16 [4, 16384, 2048], P(None, 'kv', 'tp')
The draws below stay inside these ranges and needn't reach their ends.
Inputs may be any that keep to these rules, and one draw needn't show every extreme that they name: chosen[s, b, g, 0] is b itself. Every other entry is -1 or a block index below b, and the entries of one list that are not -1 are distinct. For each block index and key group, the entries after the first slot that name that index all lie in the lists of a single sequence.
All inputs are finite; a program needn't handle non-finite values.
Results may differ from the reference program's by a relative error of at most 0.012.
The reference program's roundings to bfloat16 on the way count: a program that leaves them out, or rounds other values in their place, can miss the bound.
Values may be sent and summed in bfloat16 or wider, within the bound.
A program may use at most 64 MiB of HBM per device.

```python
import math
import jax
import jax.numpy as jnp
import numpy as np
from jax import lax

D = 2048
HEADS = 16
GROUPS = 4
HEAD_DIM = 64
CMP_STRIDE = 16
CMP_BLOCK = 32
CMP_HIDDEN = 128
SLC_BLOCK = 64
TOPK = 16
SEQS = 4
SEQ_LEN = 16384
BLOCKS = 256


def rising_columns(key):
    base = jnp.clip(jax.random.normal(key, (D, GROUPS * HEAD_DIM), jnp.float32), -4.0, 4.0) * D ** (-0.5)
    group = (jnp.arange(GROUPS * HEAD_DIM) // HEAD_DIM).astype(jnp.float32)
    factor = 3.0 ** (group / (GROUPS - 1))
    return (base * factor[None, :]).astype(jnp.bfloat16)


def draw_w_cmp_value(key, part):
    return rising_columns(jax.random.fold_in(key, 31))


def draw_w_sel_value(key, part):
    return rising_columns(jax.random.fold_in(key, 32))


def draw_hidden_in(key, part):
    shape = (SEQS, SEQ_LEN, D)
    base = jnp.clip(jax.random.normal(jax.random.fold_in(key, 41), shape, jnp.float32), -6.0, 6.0)
    return base.astype(jnp.bfloat16)


def draw_chosen(key, part):
    block_list = SEQ_LEN // SLC_BLOCK
    owner_seq = jax.random.randint(jax.random.fold_in(key, 51), (block_list, GROUPS), 0, SEQS)
    heat = jax.random.randint(jax.random.fold_in(key, 52), (block_list,), 0, 4)
    random_jitter = jax.random.randint(jax.random.fold_in(key, 53), (SEQS, block_list, GROUPS, block_list), 0, 4096)
    local_block = jnp.arange(block_list)[None, :, None, None]
    remote_block = jnp.arange(block_list)[None, None, None, :]
    seq_ids = jnp.arange(SEQS)[:, None, None, None]
    owner = jnp.transpose(owner_seq)[None, None, :, :]
    valid = (remote_block < local_block) & (owner == seq_ids)
    closest_block = jnp.max(jnp.where(valid, remote_block, -1), axis=-1, keepdims=True)
    extra_score = jnp.where(remote_block == closest_block, 1 << 20, 0) + jnp.where(remote_block == local_block - block_list // 2, 1 << 19, 0)
    weight_matrix = heat * heat * 4096
    block_score = (weight_matrix[None, None, None, :] + random_jitter + extra_score) * block_list + remote_block
    block_score = jnp.where(valid, block_score, -1 - remote_block)
    values, indices = lax.top_k(block_score, TOPK - 1)
    picked = jnp.where(values >= 0, indices, -1)
    own = jnp.broadcast_to(local_block, (SEQS, block_list, GROUPS, 1))
    return jnp.concatenate([own, picked], axis=-1).astype(jnp.int32)


def levels(rng, extent, pieces, low, top_value):
    def one(axis_at, blocks):
        draws = jax.random.uniform(jax.random.fold_in(jax.random.fold_in(rng, 6), axis_at), (blocks,), jnp.float32, low / len(pieces), top_value / len(pieces))
        return jnp.repeat(jnp.exp(draws), extent[axis_at] // blocks).reshape((-1,) + (1,) * (len(extent) - axis_at - 1))

    factor_of = one(*pieces[0])
    for cut in pieces[1:]:
        factor_of = factor_of * one(*cut)
    return factor_of


def length_profile(amount, total, limit, skew):
    loads = [(1 << 20) // math.isqrt(rank ** skew) + 1 for rank in range(2, amount + 1)]
    rest, holding = total - limit - (amount - 1), [1] * (amount - 1)
    while rest > 0:
        movable = [i for i in range(amount - 1) if holding[i] < limit]
        pool, left = sum([loads[i] for i in movable]), rest
        for i in movable:
            addition = min(limit - holding[i], max(1, left * loads[i] // pool), rest)
            holding[i] = holding[i] + addition
            rest = rest - addition
    return np.array([limit] + holding)


def ragged(own_key, amount, total, limit, slope):
    if amount == 2:
        one = jax.random.randint(own_key, (), max(1, total - limit), min(limit, total - 1) + 1)
        return jnp.stack([one, total - one])
    lengths = jnp.asarray(length_profile(amount, total, limit, slope), jnp.int32)
    couples = (amount - 1) // 2
    donor, taker = lengths[1:1 + 2 * couples:2], lengths[2:2 + 2 * couples:2]
    margin = jnp.minimum(donor - 1, limit - taker)
    moved = jax.random.randint(jax.random.fold_in(own_key, 1), (couples,), 0, 1 << 20) % (margin + 1)
    lengths = lengths.at[1:1 + 2 * couples:2].set(donor - moved).at[2:2 + 2 * couples:2].set(taker + moved)
    return lengths[jax.random.permutation(jax.random.fold_in(own_key, 2), amount)]


def normal_values(own_key, extent, deviation, most, shards=(), kind=jnp.bfloat16):
    values = jax.random.normal(own_key, extent, jnp.float32) * deviation
    if len(shards) > 0:
        values = levels(own_key, extent, shards, -0.22, 0.18) * values
    return jnp.clip(values, min=-most, max=most).astype(kind)


def setup_inputs(seed: int = 0) -> dict:
    splits = jax.random.split(jax.random.key(seed), 16)
    hidden_in = draw_hidden_in(jax.random.fold_in(splits[15], 71), 0)
    w_query = normal_values(splits[1], (D, HEADS * HEAD_DIM), D ** -0.5, 0.125, ((1, 4),))
    w_cmp_key = normal_values(splits[2], (D, GROUPS * HEAD_DIM), D ** -0.5, 0.125, ((1, 4),))
    w_cmp_value = draw_w_cmp_value(jax.random.fold_in(splits[15], 71), 0)
    w_sel_key = normal_values(splits[4], (D, GROUPS * HEAD_DIM), D ** -0.5, 0.125, ((1, 4),))
    w_sel_value = draw_w_sel_value(jax.random.fold_in(splits[15], 71), 0)
    w_gate = normal_values(splits[6], (D, 2, HEADS), D ** -0.5, 0.125)
    cmp_key_in = normal_values(splits[7], (CMP_BLOCK * HEAD_DIM, CMP_HIDDEN), (CMP_BLOCK * HEAD_DIM) ** -0.5, 0.125)
    cmp_key_out = normal_values(splits[8], (CMP_HIDDEN, HEAD_DIM), CMP_HIDDEN ** -0.5, 0.5)
    cmp_value_in = normal_values(splits[9], (CMP_BLOCK * HEAD_DIM, CMP_HIDDEN), (CMP_BLOCK * HEAD_DIM) ** -0.5, 0.125)
    cmp_value_out = normal_values(splits[10], (CMP_HIDDEN, HEAD_DIM), CMP_HIDDEN ** -0.5, 0.5)
    out_gain = jnp.clip(1.0 + 0.18 * jax.random.normal(splits[11], (HEADS * HEAD_DIM,), jnp.float32), 0.1, 1.9)
    w_out = normal_values(splits[12], (HEADS * HEAD_DIM, D), (HEADS * HEAD_DIM) ** -0.5, 0.1875)
    seq_lengths = ragged(splits[13], SEQS, SEQ_LEN + (SEQS - 1) * SEQ_LEN // 5, SEQ_LEN, 2).astype(jnp.int32)
    chosen = draw_chosen(jax.random.fold_in(splits[15], 71), 0)
    return {"hidden_in": hidden_in, "w_query": w_query, "w_cmp_key": w_cmp_key, "w_cmp_value": w_cmp_value, "w_sel_key": w_sel_key, "w_sel_value": w_sel_value, "w_gate": w_gate, "cmp_key_in": cmp_key_in, "cmp_key_out": cmp_key_out, "cmp_value_in": cmp_value_in, "cmp_value_out": cmp_value_out, "out_gain": out_gain, "w_out": w_out, "seq_lengths": seq_lengths, "chosen": chosen}


theta_base = 500000.0
norm_eps = 1e-06

def rotate(values, positions):
    width = values.shape[-1]
    half = width // 2
    inverse = jnp.exp(-jnp.log(jnp.float32(theta_base)) * jnp.arange(0, width, 2).astype(jnp.float32) / width)
    angle = positions.astype(jnp.float32)[:, None] * inverse[None, :]
    cosine = jnp.cos(angle)[:, None, :]
    sine = jnp.sin(angle)[:, None, :]
    first = values[..., :half]
    second = values[..., half:]
    return jnp.concatenate([first * cosine - second * sine, second * cosine + first * sine], axis=-1)

def masked_weights(scores, valid):
    top = lax.optimization_barrier(jnp.max(jnp.where(valid, scores, -1e+30), axis=-1, keepdims=True))
    expd = jnp.where(valid, jnp.exp(scores - top), 0.0)
    total = lax.optimization_barrier(jnp.sum(expd, axis=-1, keepdims=True))
    return (expd / jnp.maximum(total, 1.0)).astype(jnp.bfloat16)

def compress(raw, weight_in, weight_out):
    length, groups, width = raw.shape
    block_count = length // SLC_BLOCK
    per_block = SLC_BLOCK // CMP_STRIDE
    blocked = raw.reshape(block_count, SLC_BLOCK, groups, width)
    padded = jnp.concatenate([jnp.zeros((block_count, CMP_STRIDE, groups, width), raw.dtype), blocked], axis=1)
    count = block_count * per_block
    front = padded[:, :SLC_BLOCK].reshape(count, CMP_STRIDE, groups, width)
    back = padded[:, CMP_STRIDE:].reshape(count, CMP_STRIDE, groups, width)
    window = jnp.concatenate([front, back], axis=1).transpose(0, 2, 1, 3).reshape(count * groups, CMP_BLOCK * width)
    inner = jax.nn.gelu(jnp.dot(window, weight_in, preferred_element_type=jnp.float32)).astype(jnp.bfloat16)
    return jnp.dot(inner, weight_out, preferred_element_type=jnp.float32).reshape(count, groups, width)

def reference(hidden_in, w_query, w_cmp_key, w_cmp_value, w_sel_key, w_sel_value, w_gate, cmp_key_in, cmp_key_out, cmp_value_in, cmp_value_out, out_gain, w_out, seq_lengths, chosen):
    count = SEQ_LEN // CMP_STRIDE
    per_group = HEADS // GROUPS
    scale = HEAD_DIM ** (-0.5)
    entry = jnp.arange(count).astype(jnp.int32)
    ends = entry * CMP_STRIDE + CMP_STRIDE - 1

    def one_sequence(args):
        tokens, length, picks = args
        positions = jnp.arange(SEQ_LEN).astype(jnp.int32)

        def project(weight_matrix, heads):
            return jnp.dot(tokens, weight_matrix, preferred_element_type=jnp.float32).reshape(SEQ_LEN, heads, HEAD_DIM)
        queries = rotate(project(w_query, HEADS), positions).astype(jnp.bfloat16)
        sel_keys = rotate(project(w_sel_key, GROUPS), positions).astype(jnp.bfloat16)
        sel_values = project(w_sel_value, GROUPS).astype(jnp.bfloat16)
        raw_keys = project(w_cmp_key, GROUPS).astype(jnp.bfloat16)
        raw_values = project(w_cmp_value, GROUPS).astype(jnp.bfloat16)
        cmp_keys = rotate(compress(raw_keys, cmp_key_in, cmp_key_out), ends).astype(jnp.bfloat16)
        cmp_values = compress(raw_values, cmp_value_in, cmp_value_out).astype(jnp.bfloat16)
        gate_logits = jnp.dot(tokens, w_gate.reshape(D, 2 * HEADS), preferred_element_type=jnp.float32)
        gates = jax.nn.sigmoid(gate_logits).reshape(SEQ_LEN, 2, HEADS)
        cmp_key_wide = cmp_keys.astype(jnp.float32)
        cmp_value_wide = cmp_values.astype(jnp.float32)
        sel_key_wide = sel_keys.astype(jnp.float32)
        sel_value_wide = sel_values.astype(jnp.float32)
        group_ids = jnp.arange(GROUPS).astype(jnp.int32)[:, None]

        def one_block(index):
            index = index.astype(jnp.int32)
            start = index * SLC_BLOCK
            block_q = lax.dynamic_slice_in_dim(queries, start, SLC_BLOCK, 0).astype(jnp.float32)
            block_q = block_q.reshape(SLC_BLOCK, GROUPS, per_group, HEAD_DIM)
            query_pos = start + jnp.arange(SLC_BLOCK).astype(jnp.int32)
            scores = jnp.einsum('qghd,egd->ghqe', block_q, cmp_key_wide) * scale
            valid = ((entry >= 1)[None, :] & (ends[None, :] <= query_pos[:, None]))[None, None]
            weights = masked_weights(scores, valid)
            cmp_out = jnp.einsum('ghqe,egd->qghd', weights.astype(jnp.float32), cmp_value_wide)
            lists = lax.dynamic_index_in_dim(picks, index, axis=0, keepdims=False)
            safe = jnp.maximum(lists, 0)
            token = safe[:, :, None] * SLC_BLOCK + jnp.arange(SLC_BLOCK).astype(jnp.int32)[None, None, :]
            token = token.reshape(GROUPS, TOPK * SLC_BLOCK)
            keys = sel_key_wide[token, group_ids]
            values = sel_value_wide[token, group_ids]
            live = jnp.repeat(lists >= 0, SLC_BLOCK, axis=1)
            valid_s = (live[:, None, :] & (token[:, None, :] <= query_pos[None, :, None]))[:, None]
            scores_s = jnp.einsum('qghd,gmd->ghqm', block_q, keys) * scale
            weights_s = masked_weights(scores_s, valid_s)
            sel_out = jnp.einsum('ghqm,gmd->qghd', weights_s.astype(jnp.float32), values)
            block_gates = lax.dynamic_slice_in_dim(gates, start, SLC_BLOCK, 0).reshape(SLC_BLOCK, 2, GROUPS, per_group, 1)
            mixed = block_gates[:, 0] * cmp_out + block_gates[:, 1] * sel_out
            mixed = jnp.where((query_pos < length)[:, None, None, None], mixed, 0.0)
            return mixed.reshape(SLC_BLOCK, HEADS * HEAD_DIM).astype(jnp.bfloat16)
        mixed = lax.map(one_block, jnp.arange(BLOCKS).astype(jnp.int32)).reshape(SEQ_LEN, HEADS * HEAD_DIM)
        wide = mixed.astype(jnp.float32)
        scaled = (wide * out_gain[None, :]).astype(jnp.bfloat16)
        row_scale = lax.rsqrt(lax.optimization_barrier(jnp.mean(wide * wide, axis=-1, keepdims=True)) + norm_eps)
        projected = jnp.dot(scaled, w_out, preferred_element_type=jnp.float32)
        return (projected * row_scale).astype(jnp.bfloat16)
    return lax.map(one_sequence, (hidden_in, seq_lengths, chosen))
```

```python
import functools

import jax
import jax.numpy as jnp
from jax import lax
from jax.experimental import pallas as pl
from jax.experimental.pallas import tpu as pltpu
from jax.sharding import Mesh
from jax.sharding import PartitionSpec as P

HEADS = 16
HEAD_DIM = 64
CMP_STRIDE = 16
CMP_BLOCK = 32
TOPK = 16
KV = ("kv_0", "kv_1", "kv_2")
MESH = pl.DeviceIdType.MESH
ZS = 32
XS = 4
SPAN = 64
PIECE = 80
BLOCKS = 256

theta_base = 500000.0
norm_eps = 1e-06


def by_axis(array, axes):
    return functools.reduce(lax.pmax, axes, array)


def rotate(values, positions):
    width = values.shape[-1]
    half = width // 2
    inverse = jnp.exp(
        -jnp.log(jnp.float32(theta_base)) * jnp.arange(0, width, 2).astype(jnp.float32) / width
    )
    angle = positions.astype(jnp.float32)[:, None] * inverse[None, :]
    cosine = jnp.cos(angle)[:, None, :]
    sine = jnp.sin(angle)[:, None, :]
    first = values[..., :half]
    second = values[..., half:]
    return jnp.concatenate(
        [first * cosine - second * sine, second * cosine + first * sine], axis=-1
    )


def compress(raw, prior, weight_in, weight_out):
    seqs, span, groups, width = raw.shape
    extended = jnp.concatenate([prior, raw], axis=1)
    count = span // CMP_STRIDE
    front = extended[:, :span].reshape(seqs, count, CMP_STRIDE, groups, width)
    back = extended[:, CMP_STRIDE:].reshape(seqs, count, CMP_STRIDE, groups, width)
    window = jnp.concatenate([front, back], axis=2).transpose(0, 1, 3, 2, 4)
    window = window.reshape(seqs * count * groups, CMP_BLOCK * width)
    inner = jax.nn.gelu(jnp.dot(window, weight_in, preferred_element_type=jnp.float32)).astype(
        jnp.bfloat16
    )
    return jnp.dot(inner, weight_out, preferred_element_type=jnp.float32).reshape(
        seqs, count, groups, width
    )


def gather_kernel(piece, out, zsend, xsend, dsend, recv, local):
    z = lax.axis_index("kv_0")
    x = lax.axis_index("kv_1")
    c = lax.axis_index("kv_2")
    y = lax.axis_index("tp")
    right = lax.rem(x + 1, XS)
    left = lax.rem(x + XS - 1, XS)
    across = lax.rem(x + 2, XS)

    def zat(step):
        return lax.rem(z + step + ZS, ZS)

    def blk(zz, xx, cc):
        return (zz * XS + xx) * 2 + cc

    def copy(src, b, sem, device):
        return pltpu.make_async_remote_copy(
            src_ref=src,
            dst_ref=out.at[b],
            send_sem=sem,
            recv_sem=recv.at[b],
            device_id=device,
            device_id_type=MESH,
        )

    east = (z, right, c, y)
    west = (z, left, c, y)
    sibling = (z, x, 1 - c, y)

    barrier = pltpu.get_barrier_semaphore()
    partners = [(zat(s), x, c, y) for s in (1, -1, 2, -2)] + [east, west, sibling]
    for device in partners:
        pl.semaphore_signal(barrier, inc=1, device_id=device, device_id_type=MESH)
    pl.semaphore_wait(barrier, len(partners))

    me = blk(z, x, c)
    own = pltpu.make_async_copy(piece, out.at[me], local)
    own.start()
    for n, s in enumerate((1, -1, 2, -2)):
        copy(piece, me, zsend.at[n], (zat(s), x, c, y)).start()
    copy(piece, me, xsend.at[3 * z], east).start()
    copy(piece, me, xsend.at[3 * z + 1], west).start()
    copy(piece, me, dsend.at[z * XS + x], sibling).start()

    def arrive(b):
        copy(out.at[b], b, zsend.at[0], sibling).wait_recv()

    def across_core(zo, xo, b):
        copy(out.at[b], b, dsend.at[zo * XS + xo], sibling).start()

    def x_stage(zo, odd):
        b = blk(zo, left, c)
        arrive(b)
        if odd:
            copy(out.at[b], b, xsend.at[3 * zo + 2], east).start()
        across_core(zo, left, b)
        b = blk(zo, right, c)
        arrive(b)
        if not odd:
            copy(out.at[b], b, xsend.at[3 * zo + 2], west).start()
        across_core(zo, right, b)

    def o_stage(zo):
        b = blk(zo, across, c)
        arrive(b)
        across_core(zo, across, b)

    def each(r, use):
        use(2 * r - 1, 1, True)
        use(2 * r - 1, -1, True)
        use(2 * r, 1, False)

        @pl.when(r <= 7)
        def _():
            use(2 * r, -1, False)

    def body(r, carry):
        @pl.when(r <= 8)
        def _():
            def use(k, s, odd):
                zo = zat(-s * k)
                b = blk(zo, x, c)
                arrive(b)
                last = 7 if (s == 1 or odd) else 6

                @pl.when(r <= last)
                def _():
                    slot = 3 + k if s == 1 else 17 + k
                    copy(out.at[b], b, zsend.at[slot], (zat(2 * s), x, c, y)).start()

                copy(out.at[b], b, xsend.at[3 * zo], east).start()
                copy(out.at[b], b, xsend.at[3 * zo + 1], west).start()
                across_core(zo, x, b)

            each(r, use)

        @pl.when(r == 1)
        def _():
            x_stage(z, False)

        @pl.when((r >= 2) & (r <= 9))
        def _():
            each(r - 1, lambda k, s, odd: x_stage(zat(-s * k), odd))

        @pl.when(r == 2)
        def _():
            o_stage(z)

        @pl.when(r >= 3)
        def _():
            each(r - 2, lambda k, s, odd: o_stage(zat(-s * k)))

        return carry

    lax.fori_loop(1, 11, body, 0)

    def from_sibling(n, carry):
        arrive(n * 2 + 1 - c)
        return carry

    lax.fori_loop(0, ZS * XS, from_sibling, 0)
    own.wait()

    def sent(sem):
        def one(n, carry):
            copy(piece, me, sem.at[n], sibling).wait_send()
            return carry

        lax.fori_loop(0, sem.shape[0], one, 0)

    for sem in (zsend, xsend, dsend):
        sent(sem)


def gather_blocks(piece):
    sem = pltpu.SemaphoreType.DMA
    return pl.pallas_call(
        gather_kernel,
        out_shape=jax.ShapeDtypeStruct((BLOCKS, PIECE, 2 * HEAD_DIM), jnp.bfloat16),
        in_specs=[pl.BlockSpec(memory_space=pltpu.VMEM)],
        out_specs=pl.BlockSpec(memory_space=pltpu.VMEM),
        scratch_shapes=[
            sem((31,)),
            sem((3 * ZS,)),
            sem((XS * ZS,)),
            sem((BLOCKS,)),
            sem,
        ],
        compiler_params=pltpu.CompilerParams(collective_id=0, has_side_effects=True),
        name="gather_blocks",
    )(piece)


def softmax_weights(scores, valid):
    top = jnp.max(jnp.where(valid, scores, -1e30), axis=-1, keepdims=True)
    expd = jnp.where(valid, jnp.exp(scores - top), 0.0)
    total = jnp.sum(expd, axis=-1, keepdims=True)
    return (expd * (1.0 / jnp.maximum(total, 1.0))).astype(jnp.bfloat16)


NT = (((1,), (1,)), ((), ()))


def attention_kernel(place, lengths, picks, q_ref, own_ref, gate_ref, table, out, entries, pairs):
    s = pl.program_id(0)
    start = place[0] * SPAN
    count = SPAN // CMP_STRIDE
    width = 2 * HEAD_DIM

    @pl.when(s == 0)
    def _():
        def widen(n, carry):
            part = table[pl.ds(n * 16, 16), SPAN:PIECE, :]
            entries[pl.ds(n * 256, 256), :] = part.reshape(256, width).astype(jnp.float32)
            return carry

        lax.fori_loop(0, BLOCKS // 16, widen, 0)

    live = start < lengths[s]

    @pl.when(jnp.logical_not(live))
    def _():
        out[...] = jnp.zeros_like(out)

    @pl.when(live)
    def _():
        q = q_ref[0]
        rows = q.shape[0]
        cmp_pairs = jnp.concatenate(
            [
                entries[pl.ds(s * count + j, BLOCKS, stride=4 * count), :].astype(jnp.bfloat16)
                for j in range(count)
            ],
            axis=0,
        )
        total = BLOCKS * count
        scores = lax.dot_general(q, cmp_pairs, NT, preferred_element_type=jnp.float32)
        column = lax.broadcasted_iota(jnp.int32, (1, total), 1)
        entry = (column & (BLOCKS - 1)) * count + (column >> 8)
        entry_end = jnp.where(entry >= 1, entry * CMP_STRIDE + CMP_STRIDE - 1, 1 << 30)
        within = lax.broadcasted_iota(jnp.int32, (rows, 1), 0) & (SPAN - 1)
        weights = softmax_weights(scores, entry_end <= within + start)
        cmp_out = jnp.dot(weights, cmp_pairs, preferred_element_type=jnp.float32)

        pairs[0:SPAN, :] = own_ref[0]
        lane = lax.broadcasted_iota(jnp.int32, (1, TOPK * SPAN), 1)
        limit = jnp.where(lane < SPAN, lane, 0)
        for n in range(1, TOPK):
            pick = picks[s * TOPK + n]
            pairs[n * SPAN : (n + 1) * SPAN, :] = table[jnp.maximum(pick, 0), 0:SPAN, :]
            dead = jnp.where(pick < 0, 1 << 20, 0)
            limit = jnp.where((lane >> 6) == n, dead, limit)
        chosen_pairs = pairs[...]
        scores = lax.dot_general(q, chosen_pairs, NT, preferred_element_type=jnp.float32)
        weights = softmax_weights(scores, limit <= within)
        sel_out = jnp.dot(weights, chosen_pairs, preferred_element_type=jnp.float32)
        gate = gate_ref[0]
        mixed = gate[:, 0:1] * cmp_out + gate[:, 1:2] * sel_out
        mixed = jnp.where(within + start < lengths[s], mixed, 0.0).astype(jnp.bfloat16)
        mixed = mixed[:, HEAD_DIM:]
        out[0] = jnp.concatenate(
            [mixed[h * SPAN : (h + 1) * SPAN] for h in range(rows // SPAN)], axis=1
        )


def attention(place, lengths, picks, q, own, gates, table):
    seqs, rows, width = q.shape
    return pl.pallas_call(
        attention_kernel,
        out_shape=jax.ShapeDtypeStruct((seqs, SPAN, rows), jnp.bfloat16),
        grid_spec=pltpu.PrefetchScalarGridSpec(
            num_scalar_prefetch=3,
            grid=(seqs,),
            in_specs=[
                pl.BlockSpec((1, rows, width), lambda s, *_: (s, 0, 0)),
                pl.BlockSpec((1, SPAN, width), lambda s, *_: (s, 0, 0)),
                pl.BlockSpec((1, rows, 2), lambda s, *_: (s, 0, 0)),
                pl.BlockSpec(table.shape, lambda s, *_: (0, 0, 0)),
            ],
            out_specs=pl.BlockSpec((1, SPAN, rows), lambda s, *_: (s, 0, 0)),
            scratch_shapes=[
                pltpu.VMEM((BLOCKS * 16, width), jnp.float32),
                pltpu.VMEM((TOPK * SPAN, width), jnp.bfloat16),
            ],
        ),
        compiler_params=pltpu.CompilerParams(vmem_limit_bytes=48 << 20),
        name="attention",
    )(place, lengths, picks, q, own, gates, table)


def shards(
    hidden_in,
    w_query,
    w_cmp_key,
    w_cmp_value,
    w_sel_key,
    w_sel_value,
    w_gate,
    cmp_key_in,
    cmp_key_out,
    cmp_value_in,
    cmp_value_out,
    out_gain,
    w_out,
    seq_lengths,
    chosen,
):
    seqs, span, width = hidden_in.shape
    block_list = lax.axis_size(KV)
    place = lax.axis_index(KV)
    column = lax.axis_index("tp")
    local_heads = w_query.shape[1] // HEAD_DIM
    local_groups = w_sel_key.shape[1] // HEAD_DIM
    count = span // CMP_STRIDE
    scale = HEAD_DIM ** (-0.5)
    rows = hidden_in.reshape(seqs * span, width)
    positions = place * span + jnp.arange(span, dtype=jnp.int32)

    def project(weight_matrix, heads):
        return jnp.dot(rows, weight_matrix, preferred_element_type=jnp.float32).reshape(
            seqs, span, heads, HEAD_DIM
        )

    queries = rotate(project(w_query, local_heads), positions).astype(jnp.bfloat16)
    queries = jnp.transpose(queries, (0, 2, 1, 3)).reshape(seqs, local_heads * span, HEAD_DIM)
    queries = jnp.pad(queries * jnp.bfloat16(scale), ((0, 0), (0, 0), (0, HEAD_DIM)))
    sel_pairs = jnp.concatenate(
        [rotate(project(w_sel_key, local_groups), positions), project(w_sel_value, local_groups)],
        axis=-1,
    ).astype(jnp.bfloat16)
    raw_pairs = jnp.concatenate(
        [project(w_cmp_key, local_groups), project(w_cmp_value, local_groups)], axis=-1
    ).astype(jnp.bfloat16)
    prior = jnp.zeros((seqs, CMP_STRIDE, local_groups, HEAD_DIM), jnp.bfloat16)
    ends = place * span + jnp.arange(count, dtype=jnp.int32) * CMP_STRIDE + CMP_STRIDE - 1
    cmp_keys = rotate(compress(raw_pairs[..., :HEAD_DIM], prior, cmp_key_in, cmp_key_out), ends)
    cmp_values = compress(raw_pairs[..., HEAD_DIM:], prior, cmp_value_in, cmp_value_out)
    cmp_piece = jnp.concatenate(
        [cmp_keys.astype(jnp.bfloat16), cmp_values.astype(jnp.bfloat16)], axis=-1
    ).reshape(seqs * count, 2 * HEAD_DIM)
    picks = chosen[:, 0, 0]
    wanted = jnp.any(
        picks[:, 1:, None] == jnp.arange(block_list, dtype=jnp.int32), axis=1
    ).astype(jnp.int32)
    wanted = by_axis(wanted, KV)
    named = lax.dynamic_index_in_dim(wanted, place, axis=1, keepdims=False)
    seq_ids = jnp.arange(seqs, dtype=jnp.int32)
    exported_seq = jnp.sum(named * seq_ids)
    own = sel_pairs.reshape(seqs, span, 2 * HEAD_DIM)
    export = lax.dynamic_index_in_dim(own, exported_seq, axis=0, keepdims=False)
    table = gather_blocks(jnp.concatenate([export, cmp_piece], axis=0))
    gate_all = jnp.dot(rows, w_gate.reshape(width, 2 * HEADS), preferred_element_type=jnp.float32)
    gate_all = gate_all.reshape(seqs, span, 2, HEADS)
    gates = jax.nn.sigmoid(lax.dynamic_slice_in_dim(gate_all, column * local_heads, local_heads, 3))
    gates = jnp.transpose(gates, (0, 3, 1, 2)).reshape(seqs, local_heads * span, 2)
    mixed = attention(
        place.astype(jnp.int32).reshape(1), seq_lengths, picks.reshape(-1), queries, own, gates, table
    )
    mixed = mixed.reshape(seqs * span, local_heads * HEAD_DIM)
    out_width = width // lax.axis_size("tp")
    own_columns = lax.dynamic_slice_in_dim(w_out, column * out_width, out_width, 1)
    piece_wide = lax.all_gather(mixed, "tp", axis=1, tiled=True).astype(jnp.float32)
    scaled_piece = (piece_wide * out_gain[None, :]).astype(jnp.bfloat16)
    total = jnp.dot(scaled_piece, own_columns, preferred_element_type=jnp.float32)
    squares = jnp.sum(piece_wide * piece_wide, axis=-1)
    row_scale = lax.rsqrt(squares / (HEADS * HEAD_DIM) + norm_eps)
    return (total * row_scale[:, None]).astype(jnp.bfloat16).reshape(seqs, span, out_width)


def solution(mesh):
    torus = Mesh(mesh.devices.reshape(32, 4, 2, mesh.shape["tp"]), ("kv_0", "kv_1", "kv_2", "tp"))
    return jax.shard_map(
        shards,
        mesh=torus,
        in_specs=(
            P(None, KV, None),
            P(None, "tp"),
            P(None, "tp"),
            P(None, "tp"),
            P(None, "tp"),
            P(None, "tp"),
            P(),
            P(),
            P(),
            P(),
            P(),
            P(),
            P(),
            P(),
            P(None, KV, "tp", None),
        ),
        out_specs=P(None, KV, "tp"),
        check_vma=False,
    )
```
